32 devices in a mesh: sp: 16 (over z, y, x), tp: 2 (over core).
Axes of the slice: x: 2, y: 2, z: 4, core: 2. Of those that a mesh axis runs over, the one named last changes fastest.
Arguments:
- residual: bfloat16 [2048, 2048], P('sp'), may hold values from -6 to 6
- query_first: bfloat16 [2048, 8, 128], P('sp', 'tp'), may hold values from -6.5 to 6.5
- key_first: bfloat16 [2048, 8, 128], P('sp', 'tp'), may hold values from -6.5 to 6.5
- value_first: bfloat16 [2048, 8, 128], P('sp', 'tp'), may hold values from -6 to 6
- query_second: bfloat16 [2048, 8, 64], P('sp', 'tp'), may hold values from -6.5 to 6.5
- key_second: bfloat16 [2048, 8, 64], P('sp', 'tp'), may hold values from -6.5 to 6.5
- value_second: bfloat16 [2048, 8, 64], P('sp', 'tp'), may hold values from -6 to 6
- balance_first: float32 [8], P('tp'), may hold values from 0.3 to 0.8
- balance_second: float32 [8], P('tp'), may hold values from 0.3 to 0.8
- head_gain_first: float32 [128], replicated, may hold values from 0.1 to 1.9
- head_gain_second: float32 [64], replicated, may hold values from 0.1 to 1.9
- out_first: bfloat16 [1024, 2048], P('tp'), may hold values from -0.15625 to 0.15625
- out_second: bfloat16 [512, 2048], P('tp'), may hold values from -0.15625 to 0.15625
- mlp_gain: float32 [2048], replicated, may hold values from 0.1 to 1.9
- up_weight: bfloat16 [2048, 8192], P('sp', 'tp'), may hold values from -0.125 to 0.125
- down_weight: bfloat16 [2048, 8192], P('sp', 'tp'), may hold values from -0.0625 to 0.0625
Outputs:
- layer_out: bfloat16 [2048, 2048], P('sp')
The draws below stay inside these ranges and needn't reach their ends.
All inputs are finite; a program needn't handle non-finite values.
Results may differ from the reference program's by a relative error of at most 0.018.
Values may be sent and summed in bfloat16 or wider, within the bound.
A program may use at most 128 MiB of HBM per device.

```python
import math
import jax
import jax.numpy as jnp
from jax import lax

D = 2048
FF = 8192
HEADS_A = 8
HEADS_B = 8
DK_A = 64
DV_A = 128
DK_B = 32
DV_B = 64
SEQ = 2048
N_TP = 2


def drawn(key, heads, head_size):
    width = 2 * head_size
    queries = jnp.clip(1.3 * jax.random.normal(jax.random.fold_in(key, 11), (SEQ, heads, width), jnp.float32), -6.5, 6.5)
    keys = jnp.clip(1.3 * jax.random.normal(jax.random.fold_in(key, 12), (SEQ, heads, width), jnp.float32), -6.5, 6.5)
    return (queries, keys)


def draw_query_first(key, part):
    return drawn(jax.random.fold_in(key, 1), HEADS_A, DK_A)[0].astype(jnp.bfloat16)


def draw_key_first(key, part):
    return drawn(jax.random.fold_in(key, 1), HEADS_A, DK_A)[1].astype(jnp.bfloat16)


def draw_query_second(key, part):
    return drawn(jax.random.fold_in(key, 2), HEADS_B, DK_B)[0].astype(jnp.bfloat16)


def draw_key_second(key, part):
    return drawn(jax.random.fold_in(key, 2), HEADS_B, DK_B)[1].astype(jnp.bfloat16)


def block_scale(key, dims, shards, smallest, high):
    loudness = 1.0
    for position, parts in shards:
        draws = jax.random.uniform(jax.random.fold_in(jax.random.fold_in(key, 6), position), (parts,), jnp.float32, smallest / len(shards), high / len(shards))
        loudness = loudness * jnp.repeat(jnp.exp(draws), dims[position] // parts).reshape((-1,) + (1,) * (len(dims) - 1 - position))
    return loudness


def gaussian(rng, shape, spread, limit, split=(), kind=jnp.bfloat16):
    values = spread * jax.random.normal(rng, shape, jnp.float32)
    if split:
        values = values * block_scale(rng, shape, split, -0.22, 0.18)
    return jnp.clip(values, -limit, limit).astype(kind)


def setup_inputs(seed: int = 0) -> dict:
    key_list = jax.random.split(jax.random.key(seed), 17)
    return {
        "residual": gaussian(key_list[0], (SEQ, D), 1.0, 6.0, ((0, 16),)),
        "query_first": draw_query_first(jax.random.fold_in(key_list[16], 71), 0),
        "key_first": draw_key_first(jax.random.fold_in(key_list[16], 71), 0),
        "value_first": gaussian(key_list[3], (SEQ, HEADS_A, DV_A), 1.0, 6.0, ((0, 16), (1, 2))),
        "query_second": draw_query_second(jax.random.fold_in(key_list[16], 71), 0),
        "key_second": draw_key_second(jax.random.fold_in(key_list[16], 71), 0),
        "value_second": gaussian(key_list[6], (SEQ, HEADS_B, DV_B), 1.0, 6.0, ((0, 16), (1, 2))),
        "balance_first": jnp.clip(0.3 + 0.5 * jax.random.uniform(key_list[7], (HEADS_A,), jnp.float32) ** block_scale(key_list[7], (HEADS_A,), ((0, 2),), -0.2, 0.2), 0.3, 0.8),
        "balance_second": jnp.clip(0.3 + 0.5 * jax.random.uniform(key_list[8], (HEADS_B,), jnp.float32) ** block_scale(key_list[8], (HEADS_B,), ((0, 2),), -0.2, 0.2), 0.3, 0.8),
        "head_gain_first": jnp.clip(1.0 + 0.18 * jax.random.normal(key_list[9], (DV_A,), jnp.float32), 0.1, 1.9),
        "head_gain_second": jnp.clip(1.0 + 0.18 * jax.random.normal(key_list[10], (DV_B,), jnp.float32), 0.1, 1.9),
        "out_first": gaussian(key_list[11], (HEADS_A * DV_A, D), (HEADS_A * DV_A + HEADS_B * DV_B) ** -0.5, 0.15625, ((0, 2),)),
        "out_second": gaussian(key_list[12], (HEADS_B * DV_B, D), (HEADS_A * DV_A + HEADS_B * DV_B) ** -0.5, 0.15625, ((0, 2),)),
        "mlp_gain": jnp.clip(1.0 + 0.18 * jax.random.normal(key_list[13], (D,), jnp.float32), 0.1, 1.9),
        "up_weight": gaussian(key_list[14], (D, FF), D ** -0.5, 0.125, ((0, 16), (1, 2))),
        "down_weight": gaussian(key_list[15], (D, FF), FF ** -0.5, 0.0625, ((0, 16), (1, 2))),
    }


EPSILON = 1e-06
HEAD_SCALE = 0.8

def group_heads(queries, keys, values, balance, gain, head_size):
    seq = queries.shape[0]
    heads = queries.shape[1]
    depth = values.shape[2]
    block = math.gcd(256, seq)
    count = seq // block
    query_maps = queries.astype(jnp.float32).reshape(count, block, heads, 2, head_size)
    key_maps = keys.astype(jnp.float32).reshape(seq, heads, 2, head_size)
    value_float = values.astype(jnp.float32)
    columns = jnp.arange(seq, dtype=jnp.int32)
    gain_float = gain.astype(jnp.float32)

    def one_block(args):
        query_block, start = args
        scores = jnp.einsum('qhmd,khmd->hmqk', query_block, key_maps) * head_size ** (-0.5)
        positions = start + jnp.arange(block, dtype=jnp.int32)
        scores = jnp.where(columns[None, :] <= positions[:, None], scores, -jnp.inf)
        probs = jax.nn.softmax(scores, axis=-1)
        mixed = (probs[:, 0] - balance[:, None, None] * probs[:, 1]).astype(jnp.bfloat16)
        mixed = lax.optimization_barrier(mixed).astype(jnp.float32)
        summed = jnp.einsum('hqk,khe->qhe', mixed, value_float)
        power = lax.optimization_barrier(jnp.mean(summed * summed, axis=-1, keepdims=True))
        normed = summed * lax.rsqrt(power + EPSILON) * gain_float * HEAD_SCALE
        return normed.astype(jnp.bfloat16)
    starts = jnp.arange(count, dtype=jnp.int32) * block
    result = lax.map(one_block, (query_maps, starts))
    return result.reshape(seq, heads * depth)

def reference(residual, query_first, key_first, value_first, query_second, key_second, value_second, balance_first, balance_second, head_gain_first, head_gain_second, out_first, out_second, mlp_gain, up_weight, down_weight):
    heads_first = group_heads(query_first, key_first, value_first, balance_first, head_gain_first, DK_A)
    heads_second = group_heads(query_second, key_second, value_second, balance_second, head_gain_second, DK_B)
    seq = residual.shape[0]
    width = residual.shape[1]
    width_first = heads_first.shape[1] // N_TP
    width_second = heads_second.shape[1] // N_TP

    def head_part(number, total):
        offset_first = (number * width_first).astype(jnp.int32)
        offset_second = (number * width_second).astype(jnp.int32)
        part = jnp.dot(lax.dynamic_slice_in_dim(heads_first, offset_first, width_first, 1), lax.dynamic_slice_in_dim(out_first, offset_first, width_first, 0), preferred_element_type=jnp.float32)
        part = part + jnp.dot(lax.dynamic_slice_in_dim(heads_second, offset_second, width_second, 1), lax.dynamic_slice_in_dim(out_second, offset_second, width_second, 0), preferred_element_type=jnp.float32)
        rounded = lax.optimization_barrier(part.astype(jnp.bfloat16))
        return total + rounded.astype(jnp.float32)
    head_total = lax.fori_loop(0, N_TP, head_part, jnp.zeros((seq, width), jnp.float32))
    mixed = (residual.astype(jnp.float32) + head_total).astype(jnp.bfloat16)
    mixed_float = mixed.astype(jnp.float32)
    power = lax.optimization_barrier(jnp.mean(mixed_float * mixed_float, axis=-1, keepdims=True))
    normed = (mixed_float * lax.rsqrt(power + EPSILON) * mlp_gain.astype(jnp.float32)).astype(jnp.bfloat16)
    lifted = jnp.dot(normed, up_weight, preferred_element_type=jnp.float32)
    active = jax.nn.relu(lifted)
    hidden = (active * active).astype(jnp.bfloat16)
    width_hidden = hidden.shape[1] // N_TP

    def down_part(number, total):
        offset = (number * width_hidden).astype(jnp.int32)
        part = lax.dot_general(lax.dynamic_slice_in_dim(hidden, offset, width_hidden, 1), lax.dynamic_slice_in_dim(down_weight, offset, width_hidden, 1), (((1,), (1,)), ((), ())), preferred_element_type=jnp.float32)
        rounded = lax.optimization_barrier(part.astype(jnp.bfloat16))
        return total + rounded.astype(jnp.float32)
    down_total = lax.fori_loop(0, N_TP, down_part, jnp.zeros((seq, width), jnp.float32))
    return (mixed_float + down_total).astype(jnp.bfloat16)
```

```python
import functools
import math

import jax
import jax.numpy as jnp
from jax import lax
from jax.experimental import pallas as pl
from jax.experimental.pallas import tpu as pltpu
from jax.sharding import PartitionSpec as P

DK_A = 64
DK_B = 32


EPSILON = 1e-06
HEAD_SCALE = 0.8


def attend(queries, keys, values, balance, gain, device, head_size):
    tokens = queries.shape[0]
    heads = queries.shape[1]
    seq = keys.shape[0]
    depth = values.shape[2]
    block = math.gcd(512, seq)
    scale = head_size ** (-0.5)
    query_maps = queries.reshape(tokens, heads, 2, head_size)
    key_maps = keys.reshape(seq, heads, 2, head_size)
    first_row = device * tokens
    positions = first_row + jnp.arange(tokens, dtype=jnp.int32)
    needed = (first_row + tokens + block - 1) // block

    def block_scores(number):
        start = number * block
        key_block = lax.dynamic_slice_in_dim(key_maps, start, block, 0)
        scores = (
            jnp.einsum("qhmd,khmd->hmqk", query_maps, key_block, preferred_element_type=jnp.float32)
            * scale
        )
        columns = start + jnp.arange(block, dtype=jnp.int32)
        visible = columns[None, :] <= positions[:, None]
        return (jnp.where(visible, scores, -jnp.inf), start)

    def statistics(number, carry):
        highest, total = carry
        scores, start = block_scores(number)
        fresh = jnp.maximum(highest, jnp.max(scores, axis=-1, keepdims=True))
        total = total * jnp.exp(highest - fresh) + jnp.sum(
            jnp.exp(scores - fresh), axis=-1, keepdims=True
        )
        return (fresh, total)

    start_high = jnp.full((heads, 2, tokens, 1), -jnp.inf, jnp.float32)
    start_total = jnp.zeros((heads, 2, tokens, 1), jnp.float32)
    highest, total = lax.fori_loop(0, needed, statistics, (start_high, start_total))

    def accumulate(number, result):
        scores, start = block_scores(number)
        probs = jnp.exp(scores - highest) / total
        mixed = (probs[:, 0] - balance[:, None, None] * probs[:, 1]).astype(jnp.bfloat16)
        value_block = lax.dynamic_slice_in_dim(values, start, block, 0)
        return result + jnp.einsum(
            "hqk,khe->qhe", mixed, value_block, preferred_element_type=jnp.float32
        )

    summed = lax.fori_loop(0, needed, accumulate, jnp.zeros((tokens, heads, depth), jnp.float32))
    power = jnp.mean(summed * summed, axis=-1, keepdims=True)
    normed = summed * lax.rsqrt(power + EPSILON) * gain * HEAD_SCALE
    return normed.astype(jnp.bfloat16).reshape(tokens, heads * depth)


def body(
    residual,
    query_first,
    key_first,
    value_first,
    query_second,
    key_second,
    value_second,
    balance_first,
    balance_second,
    head_gain_first,
    head_gain_second,
    out_first,
    out_second,
    mlp_gain,
    up_weight,
    down_weight,
):
    device = lax.axis_index("sp")
    keys_first, values_first, keys_second, values_second = (
        lax.all_gather(key_first, "sp", axis=0, tiled=True),
        lax.all_gather(value_first, "sp", axis=0, tiled=True),
        lax.all_gather(key_second, "sp", axis=0, tiled=True),
        lax.all_gather(value_second, "sp", axis=0, tiled=True),
    )
    heads_first = attend(
        query_first, keys_first, values_first, balance_first, head_gain_first, device, DK_A
    )
    heads_second = attend(
        query_second, keys_second, values_second, balance_second, head_gain_second, device, DK_B
    )
    head_term = jnp.dot(heads_first, out_first, preferred_element_type=jnp.float32) + jnp.dot(
        heads_second, out_second, preferred_element_type=jnp.float32
    )
    head_total = lax.psum(head_term.astype(jnp.bfloat16), "tp").astype(jnp.float32)
    mixed = (residual.astype(jnp.float32) + head_total).astype(jnp.bfloat16)
    mixed_float = mixed.astype(jnp.float32)
    power = jnp.mean(mixed_float * mixed_float, axis=-1, keepdims=True)
    normed = (mixed_float * lax.rsqrt(power + EPSILON) * mlp_gain).astype(jnp.bfloat16)
    up_whole, down_whole = (
        lax.all_gather(up_weight, "sp", axis=0, tiled=True),
        lax.all_gather(down_weight, "sp", axis=0, tiled=True),
    )
    lifted = jnp.dot(normed, up_whole, preferred_element_type=jnp.float32)
    active = jax.nn.relu(lifted)
    hidden = (active * active).astype(jnp.bfloat16)
    down_term = lax.dot_general(
        hidden, down_whole, (((1,), (1,)), ((), ())), preferred_element_type=jnp.float32
    )
    added = lax.psum(down_term.astype(jnp.bfloat16), "tp").astype(jnp.float32)
    return (mixed_float + added).astype(jnp.bfloat16)


PLANE = 4
MESH = pl.DeviceIdType.MESH
VMEM_BYTES = 60 * 1024 * 1024


def remote(src, dst, send_sem, recv_sem, device):
    return pltpu.make_async_remote_copy(
        src_ref=src, dst_ref=dst, send_sem=send_sem, recv_sem=recv_sem,
        device_id=device, device_id_type=MESH,
    )


def meet(devices):
    barrier = pltpu.get_barrier_semaphore()
    for device in devices:
        pl.semaphore_signal(barrier, inc=1, device_id=device, device_id_type=MESH)
    pl.semaphore_wait(barrier, len(devices))


def places():
    s = lax.axis_index("sp")
    c = lax.axis_index("tp")
    z = s // PLANE
    p = s % PLANE
    x = p % 2
    y = p // 2
    flip_x = y * 2 + 1 - x
    flip_y = (1 - y) * 2 + x
    near = (1 - c) * flip_x + c * flip_y
    side = (1 - c) * flip_y + c * flip_x
    far = (1 - y) * 2 + 1 - x
    return s, c, z, p, near, side, far


def exchange_kernel(
    line, kv, q, up, down, kv_all, q_all, up_all, down_all,
    local, zs, zr, qs, qr, ps, pr, us, ur, ds, dr,
):
    s, c, z, p, near, side, far = places()
    n = line * PLANE
    width = up_all.shape[2]
    meet([((s + k) % n, c) for k in range(1, n)])
    own = pl.ds(pl.multiple_of(s * width, width), width)
    locals_ = [
        pltpu.make_async_copy(kv.at[z], kv_all.at[s], local.at[0]),
        pltpu.make_async_copy(q.at[z], q_all.at[z], local.at[1]),
        pltpu.make_async_copy(up.at[:, own], up_all.at[s], local.at[2]),
        pltpu.make_async_copy(down.at[:, own], down_all.at[s], local.at[3]),
    ]
    for copy in locals_:
        copy.start()
    sends = []

    def send(*args):
        copy = remote(*args)
        copy.start()
        sends.append(copy)

    for j in range(1, line):
        zt = (z + j) % line
        to = (zt * PLANE + p, c)
        send(kv.at[zt], kv_all.at[s], zs.at[j], zr.at[j], to)
        send(q.at[zt], q_all.at[z], qs.at[j], qr.at[j], to)

    def weights(ks):
        for k in ks:
            t = (s + k) % n
            columns = pl.ds(pl.multiple_of(t * width, width), width)
            send(up.at[:, columns], up_all.at[s], us.at[k], ur.at[k], (t, c))
            send(down.at[:, columns], down_all.at[s], ds.at[k], dr.at[k], (t, c))

    ring = list(range(1, n))
    share = -(-len(ring) // line)
    locals_[0].wait()
    to_near = (z * PLANE + near, c)
    to_side = (z * PLANE + side, c)
    for j in range(line):
        zf = (z + line - j) % line
        block = kv_all.at[zf * PLANE + p]
        if j:
            remote(block, block, zs.at[j], zr.at[j], to_near).wait_recv()
        send(block, block, ps.at[j, 0], pr.at[j, 0], to_near)
        send(block, block, ps.at[j, 1], pr.at[j, 1], to_side)
        weights(ring[j * share:(j + 1) * share])
    for j in range(line):
        zf = (z + line - j) % line
        block = kv_all.at[zf * PLANE + near]
        remote(block, block, ps.at[j, 0], pr.at[j, 0], to_near).wait_recv()
        send(block, block, ps.at[j, 2], pr.at[j, 2], to_side)
    for j in range(line):
        zf = (z + line - j) % line
        for way, place in ((1, side), (2, far)):
            block = kv_all.at[zf * PLANE + place]
            remote(block, block, ps.at[j, way], pr.at[j, way], to_side).wait_recv()
    for j in range(1, line):
        zf = (z + line - j) % line
        block = q_all.at[zf]
        remote(block, block, qs.at[j], qr.at[j], to_near).wait_recv()
    for k in range(1, n):
        f = (s + n - k) % n
        remote(up_all.at[f], up_all.at[f], us.at[k], ur.at[k], to_near).wait_recv()
        remote(down_all.at[f], down_all.at[f], ds.at[k], dr.at[k], to_near).wait_recv()
    for copy in locals_[1:]:
        copy.wait()
    for copy in sends:
        copy.wait_send()


def exchange(line, kv, q, up, down):
    n = line * PLANE
    width = up.shape[1] // n
    dma = pltpu.SemaphoreType.DMA
    vmem = pl.BlockSpec(memory_space=pltpu.VMEM)
    return pl.pallas_call(
        functools.partial(exchange_kernel, line),
        out_shape=(
            jax.ShapeDtypeStruct((n,) + kv.shape[1:], kv.dtype),
            jax.ShapeDtypeStruct(q.shape, q.dtype),
            jax.ShapeDtypeStruct((n, up.shape[0], width), up.dtype),
            jax.ShapeDtypeStruct((n, down.shape[0], width), down.dtype),
        ),
        in_specs=[vmem] * 4,
        out_specs=(vmem,) * 4,
        scratch_shapes=[
            dma((4,)), dma((line,)), dma((line,)), dma((line,)), dma((line,)),
            dma((line, 3)), dma((line, 3)), dma((n,)), dma((n,)), dma((n,)), dma((n,)),
        ],
        compiler_params=pltpu.CompilerParams(
            collective_id=0, has_side_effects=True, vmem_limit_bytes=32 * 1024 * 1024
        ),
    )(kv, q, up, down)


def last(a, b):
    return lax.dot_general(a, b, (((1,), (1,)), ((), ())), preferred_element_type=jnp.float32)


def attention_kernel(line, size_a, size_b, balance, q, kv, gain_a, gain_b, out):
    s, c, z, p, _, _, _ = places()
    tokens = q.shape[1]
    wide = gain_a.shape[1]
    deep = gain_b.shape[1]
    span = PLANE * tokens
    lanes = lax.broadcasted_iota(jnp.int32, (tokens, wide), 1)
    rows = lax.broadcasted_iota(jnp.int32, (tokens, span), 0) + p * tokens
    visible = lax.broadcasted_iota(jnp.int32, (tokens, span), 1) <= rows

    def mix(queries, keys_at, values_at, size, b, keys_number):
        maps = []
        for m in range(2):
            chosen = (lanes >= m * size) & (lanes < (m + 1) * size)
            picked = jnp.where(chosen, queries, jnp.zeros_like(queries))
            scores = last(picked, kv[0:keys_number, keys_at]) * size ** (-0.5)
            tail_scores = jnp.where(visible, scores[:, keys_number - span:], -jnp.inf)
            if keys_number > span:
                scores = jnp.concatenate([scores[:, : keys_number - span], tail_scores], axis=1)
            else:
                scores = tail_scores
            powers = jnp.exp(scores - jnp.max(scores, axis=-1, keepdims=True))
            maps.append((powers, jnp.sum(powers, axis=-1, keepdims=True)))
        (e1, l1), (e2, l2) = maps
        weights = (e1 * (1.0 / l1) - e2 * (b / l2)).astype(jnp.bfloat16)
        return jnp.dot(weights, kv[0:keys_number, values_at], preferred_element_type=jnp.float32)

    def norm(mixed, gain):
        power = jnp.mean(mixed * mixed, axis=-1, keepdims=True)
        return (mixed * lax.rsqrt(power + EPSILON) * gain[...] * HEAD_SCALE).astype(jnp.bfloat16)

    for j in range(line):
        number = (j + 1) * span
        first = mix(q[j, :, 0:wide], slice(0, wide), slice(wide, 2 * wide), size_a, balance[0], number)
        out[j, :, 0:wide] = norm(first, gain_a)
        both = slice(2 * wide, 3 * wide)
        second = mix(q[j, :, wide:2 * wide], both, both, size_b, balance[1], number)
        out[j, :, wide:wide + deep] = norm(second[:, wide - deep:wide], gain_b)


def attention(line, size_a, size_b, balance, q, kv, gain_a, gain_b):
    vmem = pl.BlockSpec(memory_space=pltpu.VMEM)
    shape = (line, q.shape[1], gain_a.shape[1] + gain_b.shape[1])
    return pl.pallas_call(
        functools.partial(attention_kernel, line, size_a, size_b),
        out_shape=jax.ShapeDtypeStruct(shape, jnp.bfloat16),
        in_specs=[pl.BlockSpec(memory_space=pltpu.SMEM)] + [vmem] * 4,
        out_specs=vmem,
        compiler_params=pltpu.CompilerParams(vmem_limit_bytes=32 * 1024 * 1024),
    )(balance, q, kv, gain_a, gain_b)


def return_kernel(line, heads, gathered, local, zs, zr):
    s, c, z, p, _, _, _ = places()
    meet([(((z + j) % line) * PLANE + p, c) for j in range(1, line)])
    mine = pltpu.make_async_copy(heads.at[z], gathered.at[z], local)
    mine.start()
    sends = []
    for j in range(1, line):
        zt = (z + j) % line
        copy = remote(heads.at[zt], gathered.at[z], zs.at[j], zr.at[j], (zt * PLANE + p, c))
        copy.start()
        sends.append(copy)
    for j in range(1, line):
        block = gathered.at[(z + line - j) % line]
        remote(block, block, zs.at[j], zr.at[j], (s, 1 - c)).wait_recv()
    mine.wait()
    for copy in sends:
        copy.wait_send()


def return_heads(line, heads):
    dma = pltpu.SemaphoreType.DMA
    vmem = pl.BlockSpec(memory_space=pltpu.VMEM)
    return pl.pallas_call(
        functools.partial(return_kernel, line),
        out_shape=jax.ShapeDtypeStruct(heads.shape, heads.dtype),
        in_specs=[vmem],
        out_specs=vmem,
        scratch_shapes=[dma, dma((line,)), dma((line,))],
        compiler_params=pltpu.CompilerParams(collective_id=1, has_side_effects=True),
    )(heads)


def gather_kernel(
    line, residual, part, gain, mixed, rows, other_part, xs, xr, zs, zr, ps, pr, cs, cr
):
    s, c, z, p, near, side, far = places()
    to_near = (z * PLANE + near, c)
    to_side = (z * PLANE + side, c)
    to_core = (s, 1 - c)
    meet(
        [to_near, to_side, to_core]
        + [(((z + j) % line) * PLANE + p, c) for j in range(1, line)]
    )
    swap = remote(part.at[1 - c], other_part, xs, xr, to_core)
    swap.start()
    swap.wait()
    total = part[c].astype(jnp.float32) + other_part[...].astype(jnp.float32)
    mixed[...] = (residual[c].astype(jnp.float32) + total).astype(jnp.bfloat16)
    whole = mixed[...].astype(jnp.float32)
    power = jnp.mean(whole * whole, axis=-1, keepdims=True)
    rows[s * 2 + c] = (whole * lax.rsqrt(power + EPSILON) * gain[...]).astype(jnp.bfloat16)
    sends = []

    def send(block, send_sem, recv_sem, device):
        copy = remote(block, block, send_sem, recv_sem, device)
        copy.start()
        sends.append(copy)

    def arrived(block, send_sem, recv_sem):
        remote(block, block, send_sem, recv_sem, to_core).wait_recv()

    def slot(j, place, core):
        return rows.at[(((z + line - j) % line) * PLANE + place) * 2 + core]

    for j in range(1, line):
        send(slot(0, p, c), zs.at[j], zr.at[j], (((z + j) % line) * PLANE + p, c))
    for j in range(line + 1):
        if j < line:
            block = slot(j, p, c)
            if j:
                arrived(block, zs.at[j], zr.at[j])
            send(block, ps.at[j, 0], pr.at[j, 0], to_near)
            send(block, ps.at[j, 1], pr.at[j, 1], to_side)
            send(block, cs.at[j, 0], cr.at[j, 0], to_core)
        if j:
            block = slot(j - 1, near, c)
            arrived(block, ps.at[j - 1, 0], pr.at[j - 1, 0])
            send(block, ps.at[j - 1, 2], pr.at[j - 1, 2], to_side)
            send(block, cs.at[j - 1, 1], cr.at[j - 1, 1], to_core)
    for j in range(line):
        for way, place in ((1, side), (2, far)):
            block = slot(j, place, c)
            arrived(block, ps.at[j, way], pr.at[j, way])
            send(block, cs.at[j, 1 + way], cr.at[j, 1 + way], to_core)
    for j in range(line):
        for way, place in enumerate((p, side, near, far)):
            arrived(slot(j, place, 1 - c), cs.at[j, way], cr.at[j, way])
    for copy in sends:
        copy.wait_send()


def gather_rows(line, residual, part, gain):
    dma = pltpu.SemaphoreType.DMA
    vmem = pl.BlockSpec(memory_space=pltpu.VMEM)
    _, half, features = part.shape
    return pl.pallas_call(
        functools.partial(gather_kernel, line),
        out_shape=(
            jax.ShapeDtypeStruct((half, features), jnp.bfloat16),
            jax.ShapeDtypeStruct((line * PLANE * 2, half, features), jnp.bfloat16),
        ),
        in_specs=[vmem] * 3,
        out_specs=(vmem, vmem),
        scratch_shapes=[
            pltpu.VMEM((half, features), jnp.bfloat16), dma, dma,
            dma((line,)), dma((line,)), dma((line, 3)), dma((line, 3)), dma((line, 4)), dma((line, 4)),
        ],
        compiler_params=pltpu.CompilerParams(
            collective_id=2, has_side_effects=True, vmem_limit_bytes=24 * 1024 * 1024
        ),
    )(residual, part, gain)


def scatter_kernel(
    line, terms, mixed, out, held, from_side, from_near, from_line,
    cs, cr, bs, br, as_, ar, zs, zr, fs, fr,
):
    s, c, z, p, near, side, far = places()
    to_near = (z * PLANE + near, c)
    to_side = (z * PLANE + side, c)
    to_core = (s, 1 - c)
    meet(
        [to_near, to_side, to_core]
        + [(((z + j) % line) * PLANE + p, c) for j in range(1, line)]
    )
    sends = []

    def send(*args):
        copy = remote(*args)
        copy.start()
        sends.append(copy)

    def arrived(block, send_sem, recv_sem):
        remote(block, block, send_sem, recv_sem, to_core).wait_recv()

    def add(a, b):
        return (a.astype(jnp.float32) + b.astype(jnp.float32)).astype(jnp.bfloat16)

    order = list(range(1, line)) + [0]
    for j in order:
        send(terms.at[(z + j) % line, :, 1 - c], held.at[j], cs.at[j], cr.at[j], to_core)

    def stage_core(j):
        arrived(held.at[j], cs.at[j], cr.at[j])
        zt = (z + j) % line
        for place in (side, far):
            held[j, place] = add(held[j, place], terms[zt, place, c])
        send(held.at[j, side], from_side.at[j, 0], bs.at[j, 0], br.at[j, 0], to_side)
        send(held.at[j, far], from_side.at[j, 1], bs.at[j, 1], br.at[j, 1], to_side)
        for place in (p, near):
            held[j, place] = add(held[j, place], terms[zt, place, c])

    def stage_side(j):
        arrived(from_side.at[j, 1], bs.at[j, 1], br.at[j, 1])
        held[j, near] = add(held[j, near], from_side[j, 1])
        send(held.at[j, near], from_near.at[j], as_.at[j], ar.at[j], to_near)
        arrived(from_side.at[j, 0], bs.at[j, 0], br.at[j, 0])
        held[j, p] = add(held[j, p], from_side[j, 0])

    def stage_near(j):
        arrived(from_near.at[j], as_.at[j], ar.at[j])
        held[j, p] = add(held[j, p], from_near[j])
        if j:
            send(
                held.at[j, p], from_line.at[j - 1], zs.at[j], zr.at[j],
                (((z + j) % line) * PLANE + p, c),
            )

    for step in range(line + 2):
        if step < line:
            stage_core(order[step])
        if 1 <= step <= line:
            stage_side(order[step - 1])
        if step >= 2:
            stage_near(order[step - 2])
    total = held[0, p].astype(jnp.float32)
    for j in range(1, line):
        arrived(from_line.at[j - 1], zs.at[j], zr.at[j])
        total = total + from_line[j - 1].astype(jnp.float32)
    out[c] = (mixed[...].astype(jnp.float32) + total).astype(jnp.bfloat16)
    send(out.at[c], out.at[c], fs, fr, to_core)
    arrived(out.at[1 - c], fs, fr)
    for copy in sends:
        copy.wait_send()


def scatter_sum(line, terms, mixed):
    dma = pltpu.SemaphoreType.DMA
    vmem = pl.BlockSpec(memory_space=pltpu.VMEM)
    half, features = mixed.shape
    block = (half, features)
    return pl.pallas_call(
        functools.partial(scatter_kernel, line),
        out_shape=jax.ShapeDtypeStruct((2,) + block, jnp.bfloat16),
        in_specs=[vmem] * 2,
        out_specs=vmem,
        scratch_shapes=[
            pltpu.VMEM((line, PLANE) + block, jnp.bfloat16),
            pltpu.VMEM((line, 2) + block, jnp.bfloat16),
            pltpu.VMEM((line,) + block, jnp.bfloat16),
            pltpu.VMEM((line - 1,) + block, jnp.bfloat16),
            dma((line,)), dma((line,)), dma((line, 2)), dma((line, 2)),
            dma((line,)), dma((line,)), dma((line,)), dma((line,)), dma, dma,
        ],
        compiler_params=pltpu.CompilerParams(
            collective_id=3, has_side_effects=True, vmem_limit_bytes=40 * 1024 * 1024
        ),
    )(terms, mixed)


def placed_body(
    residual, query_first, key_first, value_first, query_second, key_second, value_second,
    balance_first, balance_second, head_gain_first, head_gain_second, out_first, out_second,
    mlp_gain, up_weight, down_weight,
):
    tokens, line, wide = query_first.shape
    features = residual.shape[1]
    deep = value_second.shape[2]
    half = tokens // 2
    z = lax.axis_index("sp") // PLANE
    empty = jnp.zeros((tokens, line, wide - query_second.shape[2]), jnp.bfloat16)
    q = jnp.concatenate([query_first, query_second, empty], axis=-1).transpose(1, 0, 2)
    kv = jnp.concatenate([key_first, value_first, key_second, value_second], axis=-1)
    kv = kv.transpose(1, 0, 2)
    kv_all, q_all, up_all, down_all = exchange(line, kv, q, up_weight, down_weight)
    balance = jnp.stack([balance_first[z], balance_second[z]])
    heads = attention(
        line, wide // 2, query_second.shape[2] // 2, balance, q_all,
        kv_all.reshape(-1, kv.shape[2]), head_gain_first[None, :], head_gain_second[None, :],
    )
    heads = return_heads(line, heads)
    heads_first = heads[:, :, :wide].transpose(1, 0, 2).reshape(tokens, line * wide)
    heads_second = heads[:, :, wide:].transpose(1, 0, 2).reshape(tokens, line * deep)
    part = jnp.dot(heads_first, out_first, preferred_element_type=jnp.float32) + jnp.dot(
        heads_second, out_second, preferred_element_type=jnp.float32
    )
    part = part.astype(jnp.bfloat16).reshape(2, half, features)
    mixed, rows = gather_rows(line, residual.reshape(2, half, features), part, mlp_gain[None, :])
    up = up_all.reshape(-1, up_all.shape[2])
    down = down_all.reshape(-1, down_all.shape[2])
    lifted = jnp.dot(rows.reshape(-1, features), up, preferred_element_type=jnp.float32)
    active = jax.nn.relu(lifted)
    hidden = (active * active).astype(jnp.bfloat16)
    terms = last(hidden, down).astype(jnp.bfloat16)
    out = scatter_sum(line, terms.reshape(line, PLANE, 2, half, features), mixed)
    return out.reshape(tokens, features)


def placed(mesh):
    ranks = mesh.shape["sp"]
    cores = mesh.shape["tp"]
    return cores == 2 and ranks % PLANE == 0


def choose(mesh):
    ranks = mesh.shape["sp"]

    def run(*arrays):
        query_first, query_second, value_second, value_first = arrays[1], arrays[4], arrays[6], arrays[3]
        fits = (
            placed(mesh)
            and query_first.shape[1] * PLANE == ranks
            and query_second.shape[1] == query_first.shape[1]
            and value_first.shape[2] == query_first.shape[2] == 128
            and query_second.shape[2] + value_second.shape[2] == query_first.shape[2]
            and query_first.shape[0] % 32 == 0
            and arrays[14].shape[1] % (128 * ranks) == 0
        )
        return (placed_body if fits else body)(*arrays)

    return run


def solution(mesh):
    in_specs = (
        P("sp", None),
        P("sp", "tp", None),
        P("sp", "tp", None),
        P("sp", "tp", None),
        P("sp", "tp", None),
        P("sp", "tp", None),
        P("sp", "tp", None),
        P("tp"),
        P("tp"),
        P(),
        P(),
        P("tp", None),
        P("tp", None),
        P(),
        P("sp", "tp"),
        P("sp", "tp"),
    )
    out_specs = P("sp", None)
    return jax.shard_map(choose(mesh), mesh=mesh, in_specs=in_specs, out_specs=out_specs, check_vma=False)
```

```python
import functools
import math

import jax
import jax.numpy as jnp
from jax import lax
from jax.experimental import pallas as pl
from jax.experimental.pallas import tpu as pltpu
from jax.sharding import PartitionSpec as P

DK_A = 64
DK_B = 32


EPSILON = 1e-06
HEAD_SCALE = 0.8


def attend(queries, keys, values, balance, gain, device, head_size):
    tokens = queries.shape[0]
    heads = queries.shape[1]
    seq = keys.shape[0]
    depth = values.shape[2]
    block = math.gcd(512, seq)
    scale = head_size ** (-0.5)
    query_maps = queries.reshape(tokens, heads, 2, head_size)
    key_maps = keys.reshape(seq, heads, 2, head_size)
    first_row = device * tokens
    positions = first_row + jnp.arange(tokens, dtype=jnp.int32)
    needed = (first_row + tokens + block - 1) // block

    def block_scores(number):
        start = number * block
        key_block = lax.dynamic_slice_in_dim(key_maps, start, block, 0)
        scores = (
            jnp.einsum("qhmd,khmd->hmqk", query_maps, key_block, preferred_element_type=jnp.float32)
            * scale
        )
        columns = start + jnp.arange(block, dtype=jnp.int32)
        visible = columns[None, :] <= positions[:, None]
        return (jnp.where(visible, scores, -jnp.inf), start)

    def statistics(number, carry):
        highest, total = carry
        scores, start = block_scores(number)
        fresh = jnp.maximum(highest, jnp.max(scores, axis=-1, keepdims=True))
        total = total * jnp.exp(highest - fresh) + jnp.sum(
            jnp.exp(scores - fresh), axis=-1, keepdims=True
        )
        return (fresh, total)

    start_high = jnp.full((heads, 2, tokens, 1), -jnp.inf, jnp.float32)
    start_total = jnp.zeros((heads, 2, tokens, 1), jnp.float32)
    highest, total = lax.fori_loop(0, needed, statistics, (start_high, start_total))

    def accumulate(number, result):
        scores, start = block_scores(number)
        probs = jnp.exp(scores - highest) / total
        mixed = (probs[:, 0] - balance[:, None, None] * probs[:, 1]).astype(jnp.bfloat16)
        value_block = lax.dynamic_slice_in_dim(values, start, block, 0)
        return result + jnp.einsum(
            "hqk,khe->qhe", mixed, value_block, preferred_element_type=jnp.float32
        )

    summed = lax.fori_loop(0, needed, accumulate, jnp.zeros((tokens, heads, depth), jnp.float32))
    power = jnp.mean(summed * summed, axis=-1, keepdims=True)
    normed = summed * lax.rsqrt(power + EPSILON) * gain * HEAD_SCALE
    return normed.astype(jnp.bfloat16).reshape(tokens, heads * depth)


def body(
    residual,
    query_first,
    key_first,
    value_first,
    query_second,
    key_second,
    value_second,
    balance_first,
    balance_second,
    head_gain_first,
    head_gain_second,
    out_first,
    out_second,
    mlp_gain,
    up_weight,
    down_weight,
):
    device = lax.axis_index("sp")
    keys_first, values_first, keys_second, values_second = (
        lax.all_gather(key_first, "sp", axis=0, tiled=True),
        lax.all_gather(value_first, "sp", axis=0, tiled=True),
        lax.all_gather(key_second, "sp", axis=0, tiled=True),
        lax.all_gather(value_second, "sp", axis=0, tiled=True),
    )
    heads_first = attend(
        query_first, keys_first, values_first, balance_first, head_gain_first, device, DK_A
    )
    heads_second = attend(
        query_second, keys_second, values_second, balance_second, head_gain_second, device, DK_B
    )
    head_term = jnp.dot(heads_first, out_first, preferred_element_type=jnp.float32) + jnp.dot(
        heads_second, out_second, preferred_element_type=jnp.float32
    )
    head_total = lax.psum(head_term.astype(jnp.bfloat16), "tp").astype(jnp.float32)
    mixed = (residual.astype(jnp.float32) + head_total).astype(jnp.bfloat16)
    mixed_float = mixed.astype(jnp.float32)
    power = jnp.mean(mixed_float * mixed_float, axis=-1, keepdims=True)
    normed = (mixed_float * lax.rsqrt(power + EPSILON) * mlp_gain).astype(jnp.bfloat16)
    up_whole, down_whole = (
        lax.all_gather(up_weight, "sp", axis=0, tiled=True),
        lax.all_gather(down_weight, "sp", axis=0, tiled=True),
    )
    lifted = jnp.dot(normed, up_whole, preferred_element_type=jnp.float32)
    active = jax.nn.relu(lifted)
    hidden = (active * active).astype(jnp.bfloat16)
    down_term = lax.dot_general(
        hidden, down_whole, (((1,), (1,)), ((), ())), preferred_element_type=jnp.float32
    )
    added = lax.psum(down_term.astype(jnp.bfloat16), "tp").astype(jnp.float32)
    return (mixed_float + added).astype(jnp.bfloat16)


PLANE = 4
MESH = pl.DeviceIdType.MESH
VMEM_BYTES = 60 * 1024 * 1024


def remote(src, dst, send_sem, recv_sem, device):
    return pltpu.make_async_remote_copy(
        src_ref=src, dst_ref=dst, send_sem=send_sem, recv_sem=recv_sem,
        device_id=device, device_id_type=MESH,
    )


def meet(devices):
    barrier = pltpu.get_barrier_semaphore()
    for device in devices:
        pl.semaphore_signal(barrier, inc=1, device_id=device, device_id_type=MESH)
    pl.semaphore_wait(barrier, len(devices))


def places():
    s = lax.axis_index("sp")
    c = lax.axis_index("tp")
    z = s // PLANE
    p = s % PLANE
    x = p % 2
    y = p // 2
    flip_x = y * 2 + 1 - x
    flip_y = (1 - y) * 2 + x
    near = (1 - c) * flip_x + c * flip_y
    side = (1 - c) * flip_y + c * flip_x
    far = (1 - y) * 2 + 1 - x
    return s, c, z, p, near, side, far


def last(a, b):
    return lax.dot_general(a, b, (((1,), (1,)), ((), ())), preferred_element_type=jnp.float32)


def add(a, b):
    return (a.astype(jnp.float32) + b.astype(jnp.float32)).astype(jnp.bfloat16)


def attend_line(line, p, size_a, size_b, balance_a, balance_b, q, kv, gain_a, gain_b, out):
    tokens = q.shape[1]
    wide = gain_a.shape[1]
    deep = gain_b.shape[1]
    span = PLANE * tokens
    lanes = lax.broadcasted_iota(jnp.int32, (tokens, wide), 1)
    rows = lax.broadcasted_iota(jnp.int32, (tokens, span), 0) + p * tokens
    visible = lax.broadcasted_iota(jnp.int32, (tokens, span), 1) <= rows

    def mix(queries, keys_at, values_at, size, b, keys_number):
        maps = []
        for m in range(2):
            chosen = (lanes >= m * size) & (lanes < (m + 1) * size)
            picked = jnp.where(chosen, queries, jnp.zeros_like(queries))
            scores = last(picked, kv[0:keys_number, keys_at]) * size ** (-0.5)
            tail_scores = jnp.where(visible, scores[:, keys_number - span:], -jnp.inf)
            if keys_number > span:
                scores = jnp.concatenate([scores[:, : keys_number - span], tail_scores], axis=1)
            else:
                scores = tail_scores
            powers = jnp.exp(scores - jnp.max(scores, axis=-1, keepdims=True))
            maps.append((powers, jnp.sum(powers, axis=-1, keepdims=True)))
        (e1, l1), (e2, l2) = maps
        weights = (e1 * (1.0 / l1) - e2 * (b / l2)).astype(jnp.bfloat16)
        return jnp.dot(weights, kv[0:keys_number, values_at], preferred_element_type=jnp.float32)

    def norm(mixed, gain):
        power = jnp.mean(mixed * mixed, axis=-1, keepdims=True)
        return (mixed * lax.rsqrt(power + EPSILON) * gain[...] * HEAD_SCALE).astype(jnp.bfloat16)

    for j in range(line):
        number = (j + 1) * span
        first = mix(q[j, :, 0:wide], slice(0, wide), slice(wide, 2 * wide), size_a, balance_a, number)
        out[j, :, 0:wide] = norm(first, gain_a)
        both = slice(2 * wide, 3 * wide)
        second = mix(q[j, :, wide:2 * wide], both, both, size_b, balance_b, number)
        out[j, :, wide:wide + deep] = norm(second[:, wide - deep:wide], gain_b)


def layer_kernel(
    line, size_a, size_b, balance_a, balance_b, kv, q, gain_a, gain_b, gain, residual,
    out_a, out_b, up, down, out,
    kv_all, q_all, up_all, down_all, heads, gathered, part, other_part, mixed,
    rows, terms, held, from_side, from_near, from_line, projections_a, projections_b,
    local, kzs, kzr, qs, qr, kps, kpr, us, ur, ds, dr, hs, hr, xs, xr,
    gzs, gzr, gps, gpr, gcs, gcr, tcs, tcr, tbs, tbr, tas, tar, tzs, tzr, fs, fr,
):
    s, c, z, p, near, side, far = places()
    n = line * PLANE
    tokens = kv.shape[1]
    width = up_all.shape[1]
    depth = up.shape[0]
    half = tokens // 2
    features = residual.shape[2]
    wide = gain_a.shape[1]
    deep = gain_b.shape[1]
    to_near = (z * PLANE + near, c)
    to_side = (z * PLANE + side, c)
    to_core = (s, 1 - c)
    meet([((s + k) % n, c) for k in range(1, n)] + [to_core])
    sends = []

    def send(*args):
        copy = remote(*args)
        copy.start()
        sends.append(copy)

    def arrived(block, send_sem, recv_sem):
        remote(block, block, send_sem, recv_sem, to_core).wait_recv()

    def in_line(j):
        return (((z + j) % line) * PLANE + p, c)

    def before(j):
        return (z + line - j) % line

    def tokens_of(place):
        return kv_all.at[pl.ds(pl.multiple_of(place * tokens, tokens), tokens)]

    def share_of(ref, place):
        return ref.at[pl.ds(pl.multiple_of(place * depth, depth), depth)]

    def columns_of(place):
        return pl.ds(pl.multiple_of(place * width, width), width)

    for j in range(1, line):
        zt = (z + j) % line
        send(kv.at[zt], tokens_of(s), kzs.at[j], kzr.at[j], in_line(j))
    locals_ = [
        pltpu.make_async_copy(kv.at[z], tokens_of(s), local.at[0]),
        pltpu.make_async_copy(q.at[z], q_all.at[z], local.at[1]),
        pltpu.make_async_copy(up.at[:, columns_of(s)], share_of(up_all, s), local.at[2]),
        pltpu.make_async_copy(down.at[:, columns_of(s)], share_of(down_all, s), local.at[3]),
        pltpu.make_async_copy(out_a, projections_a, local.at[4]),
        pltpu.make_async_copy(out_b, projections_b, local.at[5]),
    ]
    for copy in locals_:
        copy.start()
    locals_[0].wait()
    for j in range(line):
        block = tokens_of(before(j) * PLANE + p)
        if j:
            arrived(block, kzs.at[j], kzr.at[j])
        send(block, block, kps.at[j, 0], kpr.at[j, 0], to_near)
        send(block, block, kps.at[j, 1], kpr.at[j, 1], to_side)
        if j == 0:
            for i in range(1, line):
                send(q.at[(z + i) % line], q_all.at[z], qs.at[i], qr.at[i], in_line(i))
            for i in range(1, line):
                k = i * PLANE
                send(
                    up.at[:, columns_of((s + k) % n)], share_of(up_all, s),
                    us.at[k], ur.at[k], ((s + k) % n, c),
                )
    for j in range(line):
        block = tokens_of(before(j) * PLANE + near)
        arrived(block, kps.at[j, 0], kpr.at[j, 0])
        send(block, block, kps.at[j, 2], kpr.at[j, 2], to_side)
    for k in range(1, n):
        if k % PLANE:
            send(
                up.at[:, columns_of((s + k) % n)], share_of(up_all, s),
                us.at[k], ur.at[k], ((s + k) % n, c),
            )
    for j in range(line):
        for way, place in ((1, side), (2, far)):
            arrived(tokens_of(before(j) * PLANE + place), kps.at[j, way], kpr.at[j, way])
    for j in range(1, line):
        arrived(q_all.at[before(j)], qs.at[j], qr.at[j])
    locals_[1].wait()

    attend_line(
        line, p, size_a, size_b, balance_a[z], balance_b[z], q_all, kv_all, gain_a, gain_b, heads
    )

    for j in range(1, line):
        send(heads.at[(z + j) % line], gathered.at[z], hs.at[j], hr.at[j], in_line(j))
    mine = pltpu.make_async_copy(heads.at[z], gathered.at[z], local.at[6])
    mine.start()
    mine.wait()
    for copy in locals_[2:]:
        copy.wait()
    for j in range(1, line):
        arrived(gathered.at[before(j)], hs.at[j], hr.at[j])
    firsts = jnp.concatenate([gathered[h, :, 0:wide] for h in range(line)], axis=1)
    seconds = jnp.concatenate([gathered[h, :, wide:wide + deep] for h in range(line)], axis=1)
    step = features // 4
    for i in range(4):
        columns = slice(i * step, (i + 1) * step)
        value = jnp.dot(firsts, projections_a[:, columns], preferred_element_type=jnp.float32)
        value = value + jnp.dot(seconds, projections_b[:, columns], preferred_element_type=jnp.float32)
        value = value.astype(jnp.bfloat16)
        part[0, :, columns] = value[:half]
        part[1, :, columns] = value[half:]
    swap = remote(part.at[1 - c], other_part, xs, xr, to_core)
    swap.start()
    swap.wait()
    total = part[c].astype(jnp.float32) + other_part[...].astype(jnp.float32)
    mixed[...] = (residual[c].astype(jnp.float32) + total).astype(jnp.bfloat16)
    whole = mixed[...].astype(jnp.float32)
    power = jnp.mean(whole * whole, axis=-1, keepdims=True)
    rows[s * 2 + c] = (whole * lax.rsqrt(power + EPSILON) * gain[...]).astype(jnp.bfloat16)

    def slot(j, place, core):
        return rows.at[(before(j) * PLANE + place) * 2 + core]

    def pass_on(block, send_sem, recv_sem, device):
        send(block, block, send_sem, recv_sem, device)

    for j in range(1, line):
        pass_on(slot(0, p, c), gzs.at[j], gzr.at[j], in_line(j))
    for j in range(line + 1):
        if j < line:
            block = slot(j, p, c)
            if j:
                arrived(block, gzs.at[j], gzr.at[j])
            pass_on(block, gps.at[j, 0], gpr.at[j, 0], to_near)
            pass_on(block, gps.at[j, 1], gpr.at[j, 1], to_side)
            pass_on(block, gcs.at[j, 0], gcr.at[j, 0], to_core)
            if j == 0:
                for k in range(1, n):
                    send(
                        down.at[:, columns_of((s + k) % n)], share_of(down_all, s),
                        ds.at[k], dr.at[k], ((s + k) % n, c),
                    )
        if j:
            block = slot(j - 1, near, c)
            arrived(block, gps.at[j - 1, 0], gpr.at[j - 1, 0])
            pass_on(block, gps.at[j - 1, 2], gpr.at[j - 1, 2], to_side)
            pass_on(block, gcs.at[j - 1, 1], gcr.at[j - 1, 1], to_core)

    def rows_here(j):
        for way, place in ((1, side), (2, far)):
            block = slot(j, place, c)
            arrived(block, gps.at[j, way], gpr.at[j, way])
            pass_on(block, gcs.at[j, 1 + way], gcr.at[j, 1 + way], to_core)

    def mixer(j):
        for way, place in enumerate((p, side, near, far)):
            arrived(slot(j, place, 1 - c), gcs.at[j, way], gcr.at[j, way])
        if j == 0:
            for k in range(1, n):
                f = (s + n - k) % n
                arrived(share_of(up_all, f), us.at[k], ur.at[k])
                arrived(share_of(down_all, f), ds.at[k], dr.at[k])
        first = before(j) * PLANE * 2
        block = rows[pl.ds(first, PLANE * 2)].reshape(PLANE * 2 * half, features)
        active = jnp.maximum(jnp.dot(block, up_all[...], preferred_element_type=jnp.float32), 0.0)
        hidden = (active * active).astype(jnp.bfloat16)
        for i in range(4):
            value = last(hidden, down_all[i * step:(i + 1) * step, :]).astype(jnp.bfloat16)
            terms[j, :, :, :, i * step:(i + 1) * step] = value.reshape(PLANE, 2, half, step)
        send(terms.at[j, :, 1 - c], held.at[j], tcs.at[j], tcr.at[j], to_core)

    def stage_core(j):
        arrived(held.at[j], tcs.at[j], tcr.at[j])
        for place in (side, far):
            held[j, place] = add(held[j, place], terms[j, place, c])
        send(held.at[j, side], from_side.at[j, 0], tbs.at[j, 0], tbr.at[j, 0], to_side)
        send(held.at[j, far], from_side.at[j, 1], tbs.at[j, 1], tbr.at[j, 1], to_side)
        for place in (p, near):
            held[j, place] = add(held[j, place], terms[j, place, c])

    def stage_side(j):
        arrived(from_side.at[j, 1], tbs.at[j, 1], tbr.at[j, 1])
        held[j, near] = add(held[j, near], from_side[j, 1])
        send(held.at[j, near], from_near.at[j], tas.at[j], tar.at[j], to_near)
        arrived(from_side.at[j, 0], tbs.at[j, 0], tbr.at[j, 0])
        held[j, p] = add(held[j, p], from_side[j, 0])

    def stage_near(j):
        arrived(from_near.at[j], tas.at[j], tar.at[j])
        held[j, p] = add(held[j, p], from_near[j])
        if j:
            send(
                held.at[j, p], from_line.at[j - 1], tzs.at[j], tzr.at[j],
                (before(j) * PLANE + p, c),
            )

    for turn in range(line + 4):
        if turn < line:
            rows_here(turn)
        if 1 <= turn <= line:
            mixer(turn - 1)
        if 2 <= turn <= line + 1:
            stage_core(turn - 2)
        if 3 <= turn <= line + 2:
            stage_side(turn - 3)
        if turn >= 4:
            stage_near(turn - 4)
    summed = held[0, p].astype(jnp.float32)
    for j in range(1, line):
        arrived(from_line.at[j - 1], tzs.at[j], tzr.at[j])
        summed = summed + from_line[j - 1].astype(jnp.float32)
    out[c] = (mixed[...].astype(jnp.float32) + summed).astype(jnp.bfloat16)
    send(out.at[c], out.at[c], fs, fr, to_core)
    arrived(out.at[1 - c], fs, fr)
    for copy in sends:
        copy.wait_send()


def layer(line, size_a, size_b, *arrays):
    kv, q, residual, out_a, out_b, up = [arrays[i] for i in (2, 3, 7, 8, 9, 10)]
    n = line * PLANE
    width = up.shape[1] // n
    _, half, features = residual.shape
    block = (half, features)
    dma = pltpu.SemaphoreType.DMA
    vmem = pl.BlockSpec(memory_space=pltpu.VMEM)
    smem = pl.BlockSpec(memory_space=pltpu.SMEM)
    hbm = pl.BlockSpec(memory_space=pl.ANY)
    wide = arrays[4].shape[1]
    deep = arrays[5].shape[1]

    def space(*shape):
        return pltpu.VMEM(shape, jnp.bfloat16)

    lines = dma((line,))
    return pl.pallas_call(
        functools.partial(layer_kernel, line, size_a, size_b),
        out_shape=jax.ShapeDtypeStruct((2,) + block, jnp.bfloat16),
        in_specs=[smem, smem] + [vmem] * 6 + [hbm] * 4,
        out_specs=vmem,
        scratch_shapes=[
            space(n * kv.shape[1], kv.shape[2]),
            space(*q.shape),
            space(n * up.shape[0], width),
            space(n * up.shape[0], width),
            space(line, q.shape[1], wide + deep),
            space(line, q.shape[1], wide + deep),
            space(2, *block),
            space(*block),
            space(*block),
            space(n * 2, *block),
            space(line, PLANE, 2, *block),
            space(line, PLANE, *block),
            space(line, 2, *block),
            space(line, *block),
            space(line - 1, *block),
            space(*out_a.shape),
            space(*out_b.shape),
            dma((7,)),
            lines, lines, lines, lines, dma((line, 3)), dma((line, 3)),
            dma((n,)), dma((n,)), dma((n,)), dma((n,)), lines, lines, dma, dma,
            lines, lines, dma((line, 3)), dma((line, 3)), dma((line, 4)), dma((line, 4)),
            lines, lines, dma((line, 2)), dma((line, 2)), lines, lines, lines, lines, dma, dma,
        ],
        compiler_params=pltpu.CompilerParams(
            collective_id=0, has_side_effects=True, vmem_limit_bytes=VMEM_BYTES
        ),
    )(*arrays)


def placed_body(
    residual, query_first, key_first, value_first, query_second, key_second, value_second,
    balance_first, balance_second, head_gain_first, head_gain_second, out_first, out_second,
    mlp_gain, up_weight, down_weight,
):
    tokens, line, wide = query_first.shape
    features = residual.shape[1]
    empty = jnp.zeros((tokens, line, wide - query_second.shape[2]), jnp.bfloat16)
    q = jnp.concatenate([query_first, query_second, empty], axis=-1).transpose(1, 0, 2)
    kv = jnp.concatenate([key_first, value_first, key_second, value_second], axis=-1)
    kv = kv.transpose(1, 0, 2)
    out = layer(
        line, wide // 2, query_second.shape[2] // 2, balance_first, balance_second, kv, q,
        head_gain_first[None, :], head_gain_second[None, :], mlp_gain[None, :],
        residual.reshape(2, tokens // 2, features), out_first, out_second, up_weight, down_weight,
    )
    return out.reshape(tokens, features)


def placed(mesh):
    ranks = mesh.shape["sp"]
    cores = mesh.shape["tp"]
    return cores == 2 and ranks % PLANE == 0


def choose(mesh):
    ranks = mesh.shape["sp"]

    def run(*arrays):
        query_first, query_second, value_second, value_first = arrays[1], arrays[4], arrays[6], arrays[3]
        fits = (
            placed(mesh)
            and query_first.shape[1] * PLANE == ranks
            and query_second.shape[1] == query_first.shape[1]
            and value_first.shape[2] == query_first.shape[2] == 128
            and query_second.shape[2] + value_second.shape[2] == query_first.shape[2]
            and query_first.shape[0] % 32 == 0
            and arrays[14].shape[1] % (128 * ranks) == 0
        )
        return (placed_body if fits else body)(*arrays)

    return run


def solution(mesh):
    in_specs = (
        P("sp", None),
        P("sp", "tp", None),
        P("sp", "tp", None),
        P("sp", "tp", None),
        P("sp", "tp", None),
        P("sp", "tp", None),
        P("sp", "tp", None),
        P("tp"),
        P("tp"),
        P(),
        P(),
        P("tp", None),
        P("tp", None),
        P(),
        P("sp", "tp"),
        P("sp", "tp"),
    )
    out_specs = P("sp", None)
    return jax.shard_map(choose(mesh), mesh=mesh, in_specs=in_specs, out_specs=out_specs, check_vma=False)
```

```python
import functools
import math

import jax
import jax.numpy as jnp
from jax import lax
from jax.experimental import pallas as pl
from jax.experimental.pallas import tpu as pltpu
from jax.sharding import PartitionSpec as P

DK_A = 64
DK_B = 32


EPSILON = 1e-06
HEAD_SCALE = 0.8


def attend(queries, keys, values, balance, gain, device, head_size):
    tokens = queries.shape[0]
    heads = queries.shape[1]
    seq = keys.shape[0]
    depth = values.shape[2]
    block = math.gcd(512, seq)
    scale = head_size ** (-0.5)
    query_maps = queries.reshape(tokens, heads, 2, head_size)
    key_maps = keys.reshape(seq, heads, 2, head_size)
    first_row = device * tokens
    positions = first_row + jnp.arange(tokens, dtype=jnp.int32)
    needed = (first_row + tokens + block - 1) // block

    def block_scores(number):
        start = number * block
        key_block = lax.dynamic_slice_in_dim(key_maps, start, block, 0)
        scores = (
            jnp.einsum("qhmd,khmd->hmqk", query_maps, key_block, preferred_element_type=jnp.float32)
            * scale
        )
        columns = start + jnp.arange(block, dtype=jnp.int32)
        visible = columns[None, :] <= positions[:, None]
        return (jnp.where(visible, scores, -jnp.inf), start)

    def statistics(number, carry):
        highest, total = carry
        scores, start = block_scores(number)
        fresh = jnp.maximum(highest, jnp.max(scores, axis=-1, keepdims=True))
        total = total * jnp.exp(highest - fresh) + jnp.sum(
            jnp.exp(scores - fresh), axis=-1, keepdims=True
        )
        return (fresh, total)

    start_high = jnp.full((heads, 2, tokens, 1), -jnp.inf, jnp.float32)
    start_total = jnp.zeros((heads, 2, tokens, 1), jnp.float32)
    highest, total = lax.fori_loop(0, needed, statistics, (start_high, start_total))

    def accumulate(number, result):
        scores, start = block_scores(number)
        probs = jnp.exp(scores - highest) / total
        mixed = (probs[:, 0] - balance[:, None, None] * probs[:, 1]).astype(jnp.bfloat16)
        value_block = lax.dynamic_slice_in_dim(values, start, block, 0)
        return result + jnp.einsum(
            "hqk,khe->qhe", mixed, value_block, preferred_element_type=jnp.float32
        )

    summed = lax.fori_loop(0, needed, accumulate, jnp.zeros((tokens, heads, depth), jnp.float32))
    power = jnp.mean(summed * summed, axis=-1, keepdims=True)
    normed = summed * lax.rsqrt(power + EPSILON) * gain * HEAD_SCALE
    return normed.astype(jnp.bfloat16).reshape(tokens, heads * depth)


def body(
    residual,
    query_first,
    key_first,
    value_first,
    query_second,
    key_second,
    value_second,
    balance_first,
    balance_second,
    head_gain_first,
    head_gain_second,
    out_first,
    out_second,
    mlp_gain,
    up_weight,
    down_weight,
):
    device = lax.axis_index("sp")
    keys_first, values_first, keys_second, values_second = (
        lax.all_gather(key_first, "sp", axis=0, tiled=True),
        lax.all_gather(value_first, "sp", axis=0, tiled=True),
        lax.all_gather(key_second, "sp", axis=0, tiled=True),
        lax.all_gather(value_second, "sp", axis=0, tiled=True),
    )
    heads_first = attend(
        query_first, keys_first, values_first, balance_first, head_gain_first, device, DK_A
    )
    heads_second = attend(
        query_second, keys_second, values_second, balance_second, head_gain_second, device, DK_B
    )
    head_term = jnp.dot(heads_first, out_first, preferred_element_type=jnp.float32) + jnp.dot(
        heads_second, out_second, preferred_element_type=jnp.float32
    )
    head_total = lax.psum(head_term.astype(jnp.bfloat16), "tp").astype(jnp.float32)
    mixed = (residual.astype(jnp.float32) + head_total).astype(jnp.bfloat16)
    mixed_float = mixed.astype(jnp.float32)
    power = jnp.mean(mixed_float * mixed_float, axis=-1, keepdims=True)
    normed = (mixed_float * lax.rsqrt(power + EPSILON) * mlp_gain).astype(jnp.bfloat16)
    up_whole, down_whole = (
        lax.all_gather(up_weight, "sp", axis=0, tiled=True),
        lax.all_gather(down_weight, "sp", axis=0, tiled=True),
    )
    lifted = jnp.dot(normed, up_whole, preferred_element_type=jnp.float32)
    active = jax.nn.relu(lifted)
    hidden = (active * active).astype(jnp.bfloat16)
    down_term = lax.dot_general(
        hidden, down_whole, (((1,), (1,)), ((), ())), preferred_element_type=jnp.float32
    )
    added = lax.psum(down_term.astype(jnp.bfloat16), "tp").astype(jnp.float32)
    return (mixed_float + added).astype(jnp.bfloat16)


PLANE = 4
MESH = pl.DeviceIdType.MESH
VMEM_BYTES = 60 * 1024 * 1024


def remote(src, dst, send_sem, recv_sem, device):
    return pltpu.make_async_remote_copy(
        src_ref=src, dst_ref=dst, send_sem=send_sem, recv_sem=recv_sem,
        device_id=device, device_id_type=MESH,
    )


def greet(devices):
    barrier = pltpu.get_barrier_semaphore()
    for device in devices:
        pl.semaphore_signal(barrier, inc=1, device_id=device, device_id_type=MESH)
    return functools.partial(pl.semaphore_wait, barrier, len(devices))


def places():
    s = lax.axis_index("sp")
    c = lax.axis_index("tp")
    z = s // PLANE
    p = s % PLANE
    x = p % 2
    y = p // 2
    flip_x = y * 2 + 1 - x
    flip_y = (1 - y) * 2 + x
    near = (1 - c) * flip_x + c * flip_y
    side = (1 - c) * flip_y + c * flip_x
    far = (1 - y) * 2 + 1 - x
    return s, c, z, p, near, side, far


def last(a, b):
    return lax.dot_general(a, b, (((1,), (1,)), ((), ())), preferred_element_type=jnp.float32)


def add(a, b):
    return (a.astype(jnp.float32) + b.astype(jnp.float32)).astype(jnp.bfloat16)


def attend_line(line, p, size_a, size_b, balance_a, balance_b, q, kv, gain_a, gain_b, out):
    tokens = q.shape[1]
    wide = gain_a.shape[1]
    deep = gain_b.shape[1]
    span = PLANE * tokens
    lanes = lax.broadcasted_iota(jnp.int32, (tokens, wide), 1)
    rows = lax.broadcasted_iota(jnp.int32, (tokens, span), 0) + p * tokens
    visible = lax.broadcasted_iota(jnp.int32, (tokens, span), 1) <= rows

    def mix(queries, keys_at, values_at, size, b, keys_number):
        maps = []
        for m in range(2):
            chosen = (lanes >= m * size) & (lanes < (m + 1) * size)
            picked = jnp.where(chosen, queries, jnp.zeros_like(queries))
            scores = last(picked, kv[0:keys_number, keys_at]) * size ** (-0.5)
            tail_scores = jnp.where(visible, scores[:, keys_number - span:], -jnp.inf)
            if keys_number > span:
                scores = jnp.concatenate([scores[:, : keys_number - span], tail_scores], axis=1)
            else:
                scores = tail_scores
            powers = jnp.exp(scores - jnp.max(scores, axis=-1, keepdims=True))
            maps.append((powers, jnp.sum(powers, axis=-1, keepdims=True)))
        (e1, l1), (e2, l2) = maps
        weights = (e1 * (1.0 / l1) - e2 * (b / l2)).astype(jnp.bfloat16)
        return jnp.dot(weights, kv[0:keys_number, values_at], preferred_element_type=jnp.float32)

    def norm(mixed, gain):
        power = jnp.mean(mixed * mixed, axis=-1, keepdims=True)
        return (mixed * lax.rsqrt(power + EPSILON) * gain[...] * HEAD_SCALE).astype(jnp.bfloat16)

    for j in range(line):
        number = (j + 1) * span
        first = mix(q[j, :, 0:wide], slice(0, wide), slice(wide, 2 * wide), size_a, balance_a, number)
        out[j, :, 0:wide] = norm(first, gain_a)
        both = slice(2 * wide, 3 * wide)
        second = mix(q[j, :, wide:2 * wide], both, both, size_b, balance_b, number)
        out[j, :, wide:wide + deep] = norm(second[:, wide - deep:wide], gain_b)


def layer_kernel(
    line, size_a, size_b, balance_a, balance_b, query_a, key_a, value_a, query_b, key_b, value_b,
    gain_a, gain_b, gain, residual, out_a, out_b, up, down, out,
    kv, q, kv_all, q_all, up_all, down_all, heads, gathered, part, other_part, mixed,
    rows, terms, held, from_side, from_near, from_line, projections_a, projections_b,
    local, kzs, kzr, qs, qr, kps, kpr, us, ur, ds, dr, hs, hr, xs, xr,
    gzs, gzr, gps, gpr, gcs, gcr, tcs, tcr, tbs, tbr, tas, tar, tzs, tzr, fs, fr,
):
    s, c, z, p, near, side, far = places()
    n = line * PLANE
    tokens = kv.shape[1]
    width = up_all.shape[1]
    depth = up.shape[0]
    half = tokens // 2
    features = residual.shape[2]
    wide = gain_a.shape[1]
    deep = gain_b.shape[1]
    to_near = (z * PLANE + near, c)
    to_side = (z * PLANE + side, c)
    to_core = (s, 1 - c)
    met = greet([((s + k) % n, c) for k in range(1, n)] + [to_core])
    for h in range(line):
        kv[h, :, 0:wide] = key_a[:, h, :]
        kv[h, :, wide:2 * wide] = value_a[:, h, :]
        kv[h, :, 2 * wide:3 * wide] = jnp.concatenate([key_b[h], value_b[h]], axis=0).T
    met()
    sends = []

    def send(*args):
        copy = remote(*args)
        copy.start()
        sends.append(copy)

    def arrived(block, send_sem, recv_sem):
        remote(block, block, send_sem, recv_sem, to_core).wait_recv()

    def in_line(j):
        return (((z + j) % line) * PLANE + p, c)

    def before(j):
        return (z + line - j) % line

    def tokens_of(place):
        return kv_all.at[pl.ds(pl.multiple_of(place * tokens, tokens), tokens)]

    def share_of(ref, place):
        return ref.at[pl.ds(pl.multiple_of(place * depth, depth), depth)]

    def columns_of(place):
        return pl.ds(pl.multiple_of(place * width, width), width)

    for j in range(1, line):
        zt = (z + j) % line
        send(kv.at[zt], tokens_of(s), kzs.at[j], kzr.at[j], in_line(j))
    locals_ = [
        pltpu.make_async_copy(kv.at[z], tokens_of(s), local.at[0]),
        pltpu.make_async_copy(q.at[z], q_all.at[z], local.at[1]),
        pltpu.make_async_copy(up.at[:, columns_of(s)], share_of(up_all, s), local.at[2]),
        pltpu.make_async_copy(down.at[:, columns_of(s)], share_of(down_all, s), local.at[3]),
        pltpu.make_async_copy(out_a, projections_a, local.at[4]),
        pltpu.make_async_copy(out_b, projections_b, local.at[5]),
    ]
    for h in range(line):
        q[h, :, 0:wide] = query_a[:, h, :]
        queries = query_b[h]
        empty = jnp.zeros((wide - queries.shape[0], tokens), queries.dtype)
        q[h, :, wide:2 * wide] = jnp.concatenate([queries, empty], axis=0).T
    for copy in locals_:
        copy.start()
    locals_[0].wait()
    for j in range(line):
        block = tokens_of(before(j) * PLANE + p)
        if j:
            arrived(block, kzs.at[j], kzr.at[j])
        send(block, block, kps.at[j, 0], kpr.at[j, 0], to_near)
        send(block, block, kps.at[j, 1], kpr.at[j, 1], to_side)
        if j == 0:
            for i in range(1, line):
                send(q.at[(z + i) % line], q_all.at[z], qs.at[i], qr.at[i], in_line(i))
            for i in range(1, line):
                k = i * PLANE
                send(
                    up.at[:, columns_of((s + k) % n)], share_of(up_all, s),
                    us.at[k], ur.at[k], ((s + k) % n, c),
                )
    for j in range(line):
        block = tokens_of(before(j) * PLANE + near)
        arrived(block, kps.at[j, 0], kpr.at[j, 0])
        send(block, block, kps.at[j, 2], kpr.at[j, 2], to_side)
    for k in range(1, n):
        if k % PLANE:
            send(
                up.at[:, columns_of((s + k) % n)], share_of(up_all, s),
                us.at[k], ur.at[k], ((s + k) % n, c),
            )
    for j in range(line):
        for way, place in ((1, side), (2, far)):
            arrived(tokens_of(before(j) * PLANE + place), kps.at[j, way], kpr.at[j, way])
    for j in range(1, line):
        arrived(q_all.at[before(j)], qs.at[j], qr.at[j])
    locals_[1].wait()

    attend_line(
        line, p, size_a, size_b, balance_a[z], balance_b[z], q_all, kv_all, gain_a, gain_b, heads
    )

    for j in range(1, line):
        send(heads.at[(z + j) % line], gathered.at[z], hs.at[j], hr.at[j], in_line(j))
    for k in range(1, n):
        send(
            down.at[:, columns_of((s + k) % n)], share_of(down_all, s),
            ds.at[k], dr.at[k], ((s + k) % n, c),
        )
    mine = pltpu.make_async_copy(heads.at[z], gathered.at[z], local.at[6])
    mine.start()
    mine.wait()
    for copy in locals_[2:]:
        copy.wait()
    for j in range(1, line):
        arrived(gathered.at[before(j)], hs.at[j], hr.at[j])
    firsts = jnp.concatenate([gathered[h, :, 0:wide] for h in range(line)], axis=1)
    seconds = jnp.concatenate([gathered[h, :, wide:wide + deep] for h in range(line)], axis=1)
    step = features // 4
    for i in range(4):
        columns = slice(i * step, (i + 1) * step)
        value = jnp.dot(firsts, projections_a[:, columns], preferred_element_type=jnp.float32)
        value = value + jnp.dot(seconds, projections_b[:, columns], preferred_element_type=jnp.float32)
        value = value.astype(jnp.bfloat16)
        part[0, :, columns] = value[:half]
        part[1, :, columns] = value[half:]
    swap = remote(part.at[1 - c], other_part, xs, xr, to_core)
    swap.start()
    swap.wait()
    total = part[c].astype(jnp.float32) + other_part[...].astype(jnp.float32)
    mixed[...] = (residual[c].astype(jnp.float32) + total).astype(jnp.bfloat16)
    whole = mixed[...].astype(jnp.float32)
    power = jnp.mean(whole * whole, axis=-1, keepdims=True)
    rows[s * 2 + c] = (whole * lax.rsqrt(power + EPSILON) * gain[...]).astype(jnp.bfloat16)

    def slot(j, place, core):
        return rows.at[(before(j) * PLANE + place) * 2 + core]

    def pass_on(block, send_sem, recv_sem, device):
        send(block, block, send_sem, recv_sem, device)

    for j in range(1, line):
        pass_on(slot(0, p, c), gzs.at[j], gzr.at[j], in_line(j))
    for j in range(line + 1):
        if j < line:
            block = slot(j, p, c)
            if j:
                arrived(block, gzs.at[j], gzr.at[j])
            pass_on(block, gps.at[j, 0], gpr.at[j, 0], to_near)
            pass_on(block, gps.at[j, 1], gpr.at[j, 1], to_side)
            pass_on(block, gcs.at[j, 0], gcr.at[j, 0], to_core)
        if j:
            block = slot(j - 1, near, c)
            arrived(block, gps.at[j - 1, 0], gpr.at[j - 1, 0])
            pass_on(block, gps.at[j - 1, 2], gpr.at[j - 1, 2], to_side)
            pass_on(block, gcs.at[j - 1, 1], gcr.at[j - 1, 1], to_core)

    def rows_here(j):
        for way, place in ((1, side), (2, far)):
            block = slot(j, place, c)
            arrived(block, gps.at[j, way], gpr.at[j, way])
            pass_on(block, gcs.at[j, 1 + way], gcr.at[j, 1 + way], to_core)

    def mixer(j):
        for way, place in enumerate((p, side, near, far)):
            arrived(slot(j, place, 1 - c), gcs.at[j, way], gcr.at[j, way])
        if j == 0:
            for k in range(1, n):
                f = (s + n - k) % n
                arrived(share_of(up_all, f), us.at[k], ur.at[k])
                arrived(share_of(down_all, f), ds.at[k], dr.at[k])
        first = before(j) * PLANE * 2
        block = rows[pl.ds(first, PLANE * 2)].reshape(PLANE * 2 * half, features)
        active = jnp.maximum(jnp.dot(block, up_all[...], preferred_element_type=jnp.float32), 0.0)
        hidden = (active * active).astype(jnp.bfloat16)
        for i in range(4):
            value = last(hidden, down_all[i * step:(i + 1) * step, :]).astype(jnp.bfloat16)
            terms[j, :, :, :, i * step:(i + 1) * step] = value.reshape(PLANE, 2, half, step)
        send(terms.at[j, :, 1 - c], held.at[j], tcs.at[j], tcr.at[j], to_core)

    def stage_core(j):
        arrived(held.at[j], tcs.at[j], tcr.at[j])
        for place in (side, far):
            held[j, place] = add(held[j, place], terms[j, place, c])
        send(held.at[j, side], from_side.at[j, 0], tbs.at[j, 0], tbr.at[j, 0], to_side)
        send(held.at[j, far], from_side.at[j, 1], tbs.at[j, 1], tbr.at[j, 1], to_side)
        for place in (p, near):
            held[j, place] = add(held[j, place], terms[j, place, c])

    def stage_side(j):
        arrived(from_side.at[j, 1], tbs.at[j, 1], tbr.at[j, 1])
        held[j, near] = add(held[j, near], from_side[j, 1])
        send(held.at[j, near], from_near.at[j], tas.at[j], tar.at[j], to_near)
        arrived(from_side.at[j, 0], tbs.at[j, 0], tbr.at[j, 0])
        held[j, p] = add(held[j, p], from_side[j, 0])

    def stage_near(j):
        arrived(from_near.at[j], tas.at[j], tar.at[j])
        held[j, p] = add(held[j, p], from_near[j])
        if j:
            send(
                held.at[j, p], from_line.at[j - 1], tzs.at[j], tzr.at[j],
                (before(j) * PLANE + p, c),
            )

    for turn in range(line + 4):
        if turn < line:
            rows_here(turn)
        if 1 <= turn <= line:
            mixer(turn - 1)
        if 2 <= turn <= line + 1:
            stage_core(turn - 2)
        if 3 <= turn <= line + 2:
            stage_side(turn - 3)
        if turn >= 4:
            stage_near(turn - 4)
    summed = held[0, p].astype(jnp.float32)
    for j in range(1, line):
        arrived(from_line.at[j - 1], tzs.at[j], tzr.at[j])
        summed = summed + from_line[j - 1].astype(jnp.float32)
    out[c] = (mixed[...].astype(jnp.float32) + summed).astype(jnp.bfloat16)
    send(out.at[c], out.at[c], fs, fr, to_core)
    arrived(out.at[1 - c], fs, fr)
    for copy in sends:
        copy.wait_send()


def layer(line, size_a, size_b, *arrays):
    query_a, residual, out_a, out_b, up = [arrays[i] for i in (2, 11, 12, 13, 14)]
    tokens = query_a.shape[0]
    n = line * PLANE
    width = up.shape[1] // n
    _, half, features = residual.shape
    block = (half, features)
    dma = pltpu.SemaphoreType.DMA
    vmem = pl.BlockSpec(memory_space=pltpu.VMEM)
    smem = pl.BlockSpec(memory_space=pltpu.SMEM)
    hbm = pl.BlockSpec(memory_space=pl.ANY)
    wide = arrays[8].shape[1]
    deep = arrays[9].shape[1]

    def space(*shape):
        return pltpu.VMEM(shape, jnp.bfloat16)

    lines = dma((line,))
    return pl.pallas_call(
        functools.partial(layer_kernel, line, size_a, size_b),
        out_shape=jax.ShapeDtypeStruct((2,) + block, jnp.bfloat16),
        in_specs=[smem, smem] + [vmem] * 10 + [hbm] * 4,
        out_specs=vmem,
        scratch_shapes=[
            space(line, tokens, 3 * wide),
            space(line, tokens, 2 * wide),
            space(n * tokens, 3 * wide),
            space(line, tokens, 2 * wide),
            space(n * up.shape[0], width),
            space(n * up.shape[0], width),
            space(line, tokens, wide + deep),
            space(line, tokens, wide + deep),
            space(2, *block),
            space(*block),
            space(*block),
            space(n * 2, *block),
            space(line, PLANE, 2, *block),
            space(line, PLANE, *block),
            space(line, 2, *block),
            space(line, *block),
            space(line - 1, *block),
            space(*out_a.shape),
            space(*out_b.shape),
            dma((7,)),
            lines, lines, lines, lines, dma((line, 3)), dma((line, 3)),
            dma((n,)), dma((n,)), dma((n,)), dma((n,)), lines, lines, dma, dma,
            lines, lines, dma((line, 3)), dma((line, 3)), dma((line, 4)), dma((line, 4)),
            lines, lines, dma((line, 2)), dma((line, 2)), lines, lines, lines, lines, dma, dma,
        ],
        compiler_params=pltpu.CompilerParams(
            collective_id=0, has_side_effects=True, vmem_limit_bytes=VMEM_BYTES
        ),
    )(*arrays)


def placed_body(
    residual, query_first, key_first, value_first, query_second, key_second, value_second,
    balance_first, balance_second, head_gain_first, head_gain_second, out_first, out_second,
    mlp_gain, up_weight, down_weight,
):
    tokens, line, wide = query_first.shape
    features = residual.shape[1]
    second = [a.transpose(1, 2, 0) for a in (query_second, key_second, value_second)]
    out = layer(
        line, wide // 2, query_second.shape[2] // 2, balance_first, balance_second,
        query_first, key_first, value_first, *second,
        head_gain_first[None, :], head_gain_second[None, :], mlp_gain[None, :],
        residual.reshape(2, tokens // 2, features), out_first, out_second, up_weight, down_weight,
    )
    return out.reshape(tokens, features)


def placed(mesh):
    ranks = mesh.shape["sp"]
    cores = mesh.shape["tp"]
    return cores == 2 and ranks % PLANE == 0


def choose(mesh):
    ranks = mesh.shape["sp"]

    def run(*arrays):
        query_first, query_second, value_second, value_first = arrays[1], arrays[4], arrays[6], arrays[3]
        fits = (
            placed(mesh)
            and query_first.shape[1] * PLANE == ranks
            and query_second.shape[1] == query_first.shape[1]
            and value_first.shape[2] == query_first.shape[2] == 128
            and query_second.shape[2] + value_second.shape[2] == query_first.shape[2]
            and query_first.shape[0] % 32 == 0
            and arrays[14].shape[1] % (128 * ranks) == 0
        )
        return (placed_body if fits else body)(*arrays)

    return run


def solution(mesh):
    in_specs = (
        P("sp", None),
        P("sp", "tp", None),
        P("sp", "tp", None),
        P("sp", "tp", None),
        P("sp", "tp", None),
        P("sp", "tp", None),
        P("sp", "tp", None),
        P("tp"),
        P("tp"),
        P(),
        P(),
        P("tp", None),
        P("tp", None),
        P(),
        P("sp", "tp"),
        P("sp", "tp"),
    )
    out_specs = P("sp", None)
    return jax.shard_map(choose(mesh), mesh=mesh, in_specs=in_specs, out_specs=out_specs, check_vma=False)
```
